32 devices in a mesh: grp: 2 (over x), ep: 8 (over z, y), tp: 2 (over core).
Axes of the slice: x: 2, y: 2, z: 4, core: 2. Of those that a mesh axis runs over, the one named last changes fastest.
Arguments:
- tokens: bfloat16 [1024, 2048], P(('grp', 'ep')), parts along dimension 0, may hold values from -6 to 6
- routes: int32 [1024, 4], P(('grp', 'ep')), parts along dimension 0, may hold values from 0 to 7, all different within a row; in each aligned block of 64 rows (0 to 63, 64 to 127, ...) at most 64 rows name the same one
- gate_weights: float32 [1024, 4], P(('grp', 'ep')), parts along dimension 0, may hold values from 0.05 to 1
- w_gate: bfloat16 [8, 2048, 1280], P('ep', None, 'tp'), may hold values from -0.125 to 0.125
- w_up: bfloat16 [8, 2048, 1280], P('ep', None, 'tp'), may hold values from -0.125 to 0.125
- w_down: bfloat16 [8, 1280, 2048], P('ep', 'tp'), may hold values from -0.15625 to 0.15625
- norm_gain: float32 [2048], P('tp'), may hold values from 0.1 to 1.9
- norm_bias: float32 [2048], P('tp'), may hold values from -2 to 2
Outputs:
- normed: bfloat16 [1024, 2048], P(('grp', 'ep'), 'tp'), parts along dimension 0
The draws below stay inside these ranges and needn't reach their ends.
There are 2 independent parts, one for each index of `grp`. The reference program is written for one: setup_inputs(seed, part) draws one part's arguments, and reference() takes and returns one part's arrays. A program takes and returns all parts, laid end to end along the dimension named above; an argument that names none is the same for every part. Nothing has to cross between parts.
Inputs may be any that keep to these rules, and one draw needn't show every extreme that they name: `routes`: the rows of a token name distinct experts; in each aligned block of 64 rows (the tokens of one index of ep) no expert is named more than 64 times, a bound that some block reaches.
All inputs are finite; a program needn't handle non-finite values.
Results may differ from the reference program's by a relative error of at most 0.0037.
Values may be sent and summed in bfloat16 or wider, within the bound.
A program may use at most 64 MiB of HBM per device.

```python
import math
import jax
import jax.numpy as jnp
import numpy as np
from jax import lax

D = 2048
FF = 1280
TOP = 4
TOK_DEV = 64
EXPERTS = 8
CAP = 64
TOKENS = 512
N_EP = 8
N_TP = 2


def block_scale(key, extent, split, low, high):
    def one(position, blocks):
        draws = jax.random.uniform(jax.random.fold_in(jax.random.fold_in(key, 6), position), (blocks,), jnp.float32, low / len(split), high / len(split))
        return jnp.repeat(jnp.exp(draws), extent[position] // blocks).reshape((-1,) + (1,) * (len(extent) - position - 1))

    level = one(*split[0])
    for cut in split[1:]:
        level = level * one(*cut)
    return level


def routed_block(key, own, number, rows, count, top, reach, lean):
    sequence = jax.random.permutation(key, count)
    crowded, usual = portions_of(count, rows * top, reach, lean, True), portions_of(count, rows * top, reach, lean, False)
    places = jnp.arange(count)

    def named(lengths, rotation):
        used = int((lengths > 0).sum())
        fixed = max(1, used // 4)
        shifted = fixed + (places - fixed + rotation * (used - fixed)) % max(1, count - fixed)
        return jnp.zeros((count,), jnp.int32).at[sequence[jnp.where(places < fixed, places, shifted)]].set(jnp.asarray(lengths, jnp.int32))

    lengths = jnp.where(number % 4 == 0, named(crowded, number // 4), named(usual, number - number // 4 - 1))
    mixed = jax.random.permutation(jax.random.fold_in(own, 3), count)
    donor, taker = mixed[0:count // 2 * 2:2], mixed[1:count // 2 * 2:2]
    room = jnp.minimum(lengths[donor] - 1, reach - lengths[taker]) // 2
    room = jnp.where((donor == sequence[0]) | (taker == sequence[0]) | (lengths[taker] == 0), 0, jnp.maximum(room, 0))
    shifted = jax.random.randint(jax.random.fold_in(own, 4), (count // 2,), 0, 1 << 20) % (room + 1)
    lengths = lengths.at[donor].add(-shifted).at[taker].add(shifted)
    items = jnp.searchsorted(jnp.cumsum(lengths), jnp.arange(rows * top), side="right").astype(jnp.int32)
    grid = items.reshape(top, rows).T
    grid = grid[jax.random.permutation(jax.random.fold_in(own, 1), rows)]
    rotation = jax.random.randint(jax.random.fold_in(own, 2), (rows, 1), 0, top)
    return jnp.take_along_axis(grid, (jnp.arange(top)[None, :] + rotation) % top, axis=1)


def portions_of(amount, total, limit, skew, full):
    portions = [(1 << 20) // math.isqrt(rank ** skew) + 1 for rank in range(1, amount + 1)]
    largest = limit if full else min(limit, max(-(-total // amount), total * portions[0] // sum(portions)))
    least = 1 if total - largest >= amount - 1 else 0
    given, rest = [largest] + [least] * (amount - 1), total - largest - least * (amount - 1)
    while rest > 0:
        movable = [i for i in range(1, amount) if given[i] < largest] or [i for i in range(1, amount) if given[i] < limit]
        whole, left = sum([portions[i] for i in movable]), rest
        for i in movable:
            addition = min(limit - given[i], max(1, left * portions[i] // whole), rest)
            given[i] = given[i] + addition
            rest = rest - addition
    return np.array(given)


def gaussian(rng, dims, deviation, bound, pieces=(), kind=jnp.bfloat16):
    values = deviation * jax.random.normal(rng, dims, jnp.float32)
    if pieces:
        values = values * block_scale(rng, dims, pieces, -0.22, 0.18)
    return jnp.clip(values, -bound, bound).astype(kind)


def setup_inputs(seed: int = 0, part: int = 0) -> dict:
    streams_of = jax.random.split(jax.random.key(seed), 9)
    own_keys = jax.random.split(jax.random.fold_in(streams_of[8], part), 9)
    tokens = gaussian(own_keys[0], (TOKENS, D), 1.0, 6.0, ((0, 8),))
    routes_keys = jax.random.split(jax.random.fold_in(own_keys[1], 1), TOKENS // TOK_DEV)
    routes_turns = jax.random.permutation(jax.random.fold_in(own_keys[1], 3), TOKENS // TOK_DEV)
    routes = jax.vmap(lambda own, number: routed_block(jax.random.fold_in(own_keys[1], 2), own, number, TOK_DEV, EXPERTS, TOP, CAP, 2))(routes_keys, routes_turns).reshape((TOKENS, TOP))
    gate_weights = jnp.clip(jnp.exp(math.log(1.0) - 2.9957323 * jax.random.uniform(own_keys[2], (TOKENS, TOP), jnp.float32) ** block_scale(own_keys[2], (TOKENS, TOP), ((0, 8),), -0.2, 0.2)), 0.05, 1.0)
    w_gate = gaussian(streams_of[3], (EXPERTS, D, FF), D ** -0.5, 0.125, ((0, 8), (2, 2)))
    w_up = gaussian(streams_of[4], (EXPERTS, D, FF), D ** -0.5, 0.125, ((0, 8), (2, 2)))
    w_down = gaussian(streams_of[5], (EXPERTS, FF, D), FF ** -0.5, 0.15625, ((0, 8), (1, 2)))
    norm_gain = jnp.clip(1.0 + 0.18 * jax.random.normal(streams_of[6], (D,), jnp.float32), 0.1, 1.9)
    norm_bias = gaussian(streams_of[7], (D,), 0.4, 2.0, ((0, 2),), jnp.float32)
    return {"tokens": tokens, "routes": routes, "gate_weights": gate_weights, "w_gate": w_gate, "w_up": w_up, "w_down": w_down, "norm_gain": norm_gain, "norm_bias": norm_bias}


residual_scale = 1.4142135
norm_eps = 1e-05

def reference(tokens, routes, gate_weights, w_gate, w_up, w_down, norm_gain, norm_bias):
    pair_list = routes.reshape(N_EP, TOK_DEV * TOP).astype(jnp.int32)
    onehot = (pair_list[..., None] == jnp.arange(EXPERTS, dtype=jnp.int32)).astype(jnp.int32)
    slots = lax.optimization_barrier(jnp.sum((jnp.cumsum(onehot, axis=1) - onehot) * onehot, axis=-1))
    blocks = tokens.reshape(N_EP, TOK_DEV, D).astype(jnp.float32)
    weights = gate_weights.reshape(N_EP, TOK_DEV, TOP).astype(jnp.float32)
    columns = jnp.arange(CAP, dtype=jnp.int32)
    half = FF // N_TP

    def one_expert(carry, inputs):
        expert, gate_w, up_w, down_w = inputs
        picked = ((pair_list == expert)[..., None] & (slots[..., None] == columns)).astype(jnp.float32)
        picked = picked.reshape(N_EP, TOK_DEV, TOP, CAP)
        placed = lax.optimization_barrier(jnp.sum(picked, axis=2))
        rows = jnp.einsum('stc,std->scd', placed, blocks, precision=lax.Precision.HIGHEST)
        rows = rows.astype(jnp.bfloat16).reshape(N_EP * CAP, D)
        gate = jnp.dot(rows, gate_w, preferred_element_type=jnp.float32)
        upper = jnp.dot(rows, up_w, preferred_element_type=jnp.float32)
        hidden = (jax.nn.silu(gate) * upper).astype(jnp.bfloat16)
        total = jnp.zeros((N_EP * CAP, D), jnp.float32)
        for index in range(N_TP):
            partial_sum = jnp.dot(hidden[:, index * half:(index + 1) * half], down_w[index * half:(index + 1) * half], preferred_element_type=jnp.float32)
            total = total + lax.optimization_barrier(partial_sum.astype(jnp.bfloat16)).astype(jnp.float32)
        output = lax.optimization_barrier(total.astype(jnp.bfloat16)).astype(jnp.float32)
        output = output.reshape(N_EP, CAP, D)
        mixing = jnp.einsum('stkc,stk->stc', picked, weights, precision=lax.Precision.HIGHEST)
        carry = carry + jnp.einsum('stc,scd->std', mixing, output, precision=lax.Precision.HIGHEST)
        return (carry, None)
    start = jnp.zeros((N_EP, TOK_DEV, D), jnp.float32)
    mixed, _ = lax.scan(one_expert, start, (jnp.arange(EXPERTS, dtype=jnp.int32), w_gate, w_up, w_down))
    mixture = lax.optimization_barrier(mixed.reshape(TOKENS, D).astype(jnp.bfloat16)).astype(jnp.float32)
    summed = residual_scale * tokens.astype(jnp.float32) + mixture
    mean = lax.optimization_barrier(jnp.mean(summed, axis=-1, keepdims=True))
    variance = lax.optimization_barrier(jnp.mean(jnp.square(summed - mean), axis=-1, keepdims=True))
    normed = (summed - mean) * lax.rsqrt(variance + norm_eps) * norm_gain + norm_bias
    return normed.astype(jnp.bfloat16)
```

```python
import functools
import jax
import jax.numpy as jnp
from jax import lax
from jax.experimental import pallas as pl
from jax.experimental.pallas import tpu as pltpu
from jax.sharding import PartitionSpec as P

residual_scale = 1.4142135
norm_eps = 1e-05
MESH = pl.DeviceIdType.MESH
LANES = 128


def kernel(n, num_tp, tokens, routes, weights, gain, bias, wg_hbm, wu_hbm, wd_hbm, out,
           xs, wg, wu, wd, own, part_out, part_in, ret_out, ret_in, stat_out, stat_in,
           w_sem, gs, gr, fs, fr, ps, pr, rs, rr, ss, sr):
    me = lax.axis_index("ep")
    core = lax.axis_index("tp")
    other = lax.rem(core + 1, num_tp)
    rows, width = tokens.shape
    half = width // num_tp
    share = rows // num_tp
    pairs = n // 2
    z, y = me // 2, lax.rem(me, 2)
    partner = 2 * z + 1 - y
    my_rows = pl.ds(pl.multiple_of(core * share, share), share)
    my_cols = pl.ds(pl.multiple_of(core * half, half), half)
    other_cols = pl.ds(pl.multiple_of(other * half, half), half)

    loads = [pltpu.make_async_copy(a.at[0], b, w_sem.at[i])
             for i, (a, b) in enumerate(((wg_hbm, wg), (wu_hbm, wu), (wd_hbm, wd)))]
    for load in loads:
        load.start()

    barrier = pltpu.get_barrier_semaphore()
    for k in range(1, n):
        pl.semaphore_signal(barrier, inc=1, device_id={"ep": lax.rem(me + k, n)}, device_id_type=MESH)
    pl.semaphore_signal(barrier, inc=1, device_id={"tp": other}, device_id_type=MESH)
    xs[me] = tokens[...]
    pl.semaphore_wait(barrier, n)

    def offset(g):
        step = (g + 1) // 2
        return step * (2 * lax.rem(g, 2) - 1)

    def ahead(g):
        return lax.rem(z + offset(g) + pairs, pairs)

    def behind(g):
        return lax.rem(z - offset(g) + pairs, pairs)

    def gather_copy(target, source):
        return pltpu.make_async_remote_copy(
            src_ref=tokens.at[my_rows, :], dst_ref=xs.at[source, my_rows, :],
            send_sem=gs.at[target], recv_sem=gr.at[source],
            device_id={"ep": target}, device_id_type=MESH)

    def forward_copy(source, who):
        part = pl.ds(pl.multiple_of(who * share, share), share)
        return pltpu.make_async_remote_copy(
            src_ref=xs.at[source, part, :], dst_ref=xs.at[source, part, :],
            send_sem=fs.at[source], recv_sem=fr.at[source],
            device_id={"tp": other}, device_id_type=MESH)

    def partial_copy(zz):
        block = pl.ds(2 * zz, 2)
        return pltpu.make_async_remote_copy(
            src_ref=part_out.at[block], dst_ref=part_in.at[block],
            send_sem=ps.at[zz], recv_sem=pr.at[zz],
            device_id={"tp": other}, device_id_type=MESH)

    def return_copy(target, source):
        return pltpu.make_async_remote_copy(
            src_ref=ret_out.at[target], dst_ref=ret_in.at[source],
            send_sem=rs.at[target], recv_sem=rr.at[source],
            device_id={"ep": target}, device_id_type=MESH)

    gather_copy(partner, me).start()

    def send_tokens(g, carry):
        zz = behind(g)
        gather_copy(2 * zz + y, me).start()
        gather_copy(2 * zz + 1 - y, me).start()
        return carry

    lax.fori_loop(1, pairs, send_tokens, 0)

    def pass_on(source):
        gather_copy(partner, source).wait_recv()
        forward_copy(source, core).start()

    def finish(g):
        zz = ahead(g)
        partial_copy(zz).wait_recv()
        block = pl.ds(2 * zz, 2)
        total = own[block] + part_in[block].astype(jnp.float32)
        ret_out[block] = total.astype(jnp.bfloat16)

    def step(i, carry):
        @pl.when(i == 0)
        def _():
            pass_on(partner)

        @pl.when((i > 0) & (i < pairs))
        def _():
            zz = ahead(i)
            pass_on(2 * zz + y)
            pass_on(2 * zz + 1 - y)

        @pl.when(i == 1)
        def _():
            for load in loads:
                load.wait()
            forward_copy(partner, other).wait_recv()

        @pl.when((i > 1) & (i <= pairs))
        def _():
            zz = ahead(i - 1)
            forward_copy(2 * zz, other).wait_recv()
            forward_copy(2 * zz + 1, other).wait_recv()

        @pl.when((i > 0) & (i <= pairs))
        def _():
            zz = ahead(i - 1)
            block = pl.ds(2 * zz, 2)
            x = xs[block].reshape(2 * rows, width)
            gate = jnp.dot(x, wg[...], preferred_element_type=jnp.float32)
            upper = jnp.dot(x, wu[...], preferred_element_type=jnp.float32)
            hidden = (gate / (1.0 + jnp.exp(-gate)) * upper).astype(jnp.bfloat16)
            theirs = jnp.dot(hidden, wd[:, other_cols], preferred_element_type=jnp.float32)
            part_out[block] = theirs.astype(jnp.bfloat16).reshape(2, rows, half)
            partial_copy(zz).start()
            mine = jnp.dot(hidden, wd[:, my_cols], preferred_element_type=jnp.float32)
            own[block] = mine.reshape(2, rows, half)

        @pl.when(i == 2)
        def _():
            finish(0)
            return_copy(partner, me).start()

        @pl.when(i > 2)
        def _():
            finish(i - 2)
            zz = ahead(i - 2)
            return_copy(2 * zz + y, me).start()
            return_copy(2 * zz + 1 - y, me).start()

        return carry

    lax.fori_loop(0, pairs + 2, step, 0)

    route = routes[...]
    weight = weights[...]

    def weighted(source, block):
        w = jnp.sum(jnp.where(route == source, weight, 0.0), axis=1, keepdims=True)
        return w * block.astype(jnp.float32)

    return_copy(partner, partner).wait_recv()
    own[0] = weighted(me, ret_out[me]) + weighted(partner, ret_in[partner])

    def collect(g, carry):
        zz = behind(g)
        return_copy(partner, 2 * zz + y).wait_recv()
        return_copy(partner, 2 * zz + 1 - y).wait_recv()
        own[0] = own[0] + weighted(2 * zz, ret_in[2 * zz]) + weighted(2 * zz + 1, ret_in[2 * zz + 1])
        return carry

    lax.fori_loop(1, pairs, collect, 0)
    mixture = own[0].astype(jnp.bfloat16).astype(jnp.float32)
    summed = residual_scale * tokens[:, my_cols].astype(jnp.float32) + mixture
    row_sum = jnp.sum(summed, axis=1, keepdims=True)
    row_squares = jnp.sum(summed * summed, axis=1, keepdims=True)
    lane = lax.broadcasted_iota(jnp.int32, (rows, LANES), 1)
    stat_out[...] = jnp.where(lane == 0, row_sum, row_squares)
    stats = pltpu.make_async_remote_copy(
        src_ref=stat_out, dst_ref=stat_in, send_sem=ss, recv_sem=sr,
        device_id={"tp": other}, device_id_type=MESH)
    stats.start()

    gather_copy(partner, me).wait_send()
    forward_copy(partner, core).wait_send()
    partial_copy(z).wait_send()
    return_copy(partner, me).wait_send()

    def drain(g, carry):
        zz = ahead(g)
        partial_copy(zz).wait_send()
        for j in range(2):
            gather_copy(2 * zz + j, me).wait_send()
            forward_copy(2 * zz + j, core).wait_send()
            return_copy(2 * zz + j, me).wait_send()
        return carry

    lax.fori_loop(1, pairs, drain, 0)
    stats.wait()
    row_sum = row_sum + stat_in[:, 0:1]
    row_squares = row_squares + stat_in[:, 1:2]
    mean = row_sum / width
    variance = row_squares / width - mean * mean
    normed = (summed - mean) * lax.rsqrt(variance + norm_eps) * gain[...] + bias[...]
    out[...] = normed.astype(jnp.bfloat16)


def shards(n, num_tp, tokens, routes, gate_weights, w_gate, w_up, w_down, norm_gain, norm_bias):
    rows, width = tokens.shape
    hidden = w_gate.shape[2]
    half = width // num_tp
    vmem = pl.BlockSpec(memory_space=pltpu.VMEM)
    hbm = pl.BlockSpec(memory_space=pl.ANY)
    dma = pltpu.SemaphoreType.DMA
    return pl.pallas_call(
        functools.partial(kernel, n, num_tp),
        out_shape=jax.ShapeDtypeStruct((rows, half), jnp.bfloat16),
        in_specs=[vmem] * 5 + [hbm] * 3,
        out_specs=vmem,
        scratch_shapes=[
            pltpu.VMEM((n, rows, width), jnp.bfloat16),
            pltpu.VMEM((width, hidden), jnp.bfloat16),
            pltpu.VMEM((width, hidden), jnp.bfloat16),
            pltpu.VMEM((hidden, width), jnp.bfloat16),
            pltpu.VMEM((n, rows, half), jnp.float32),
            pltpu.VMEM((n, rows, half), jnp.bfloat16),
            pltpu.VMEM((n, rows, half), jnp.bfloat16),
            pltpu.VMEM((n, rows, half), jnp.bfloat16),
            pltpu.VMEM((n, rows, half), jnp.bfloat16),
            pltpu.VMEM((rows, LANES), jnp.float32),
            pltpu.VMEM((rows, LANES), jnp.float32),
            dma((3,)), dma((n,)), dma((n,)), dma((n,)), dma((n,)), dma((n // 2,)), dma((n // 2,)),
            dma((n,)), dma((n,)), dma, dma,
        ],
        compiler_params=pltpu.CompilerParams(collective_id=0, has_side_effects=True),
    )(tokens, routes, gate_weights, norm_gain.reshape(1, half), norm_bias.reshape(1, half),
      w_gate, w_up, w_down)


def solution(mesh):
    in_specs = (
        P(("grp", "ep"), None),
        P(("grp", "ep"), None),
        P(("grp", "ep"), None),
        P("ep", None, "tp"),
        P("ep", None, "tp"),
        P("ep", "tp", None),
        P("tp"),
        P("tp"),
    )
    out_specs = P(("grp", "ep"), "tp")
    body = functools.partial(shards, mesh.shape["ep"], mesh.shape["tp"])
    return jax.shard_map(body, mesh=mesh, in_specs=in_specs, out_specs=out_specs, check_vma=False)
```

```python
import functools
import jax
import jax.numpy as jnp
from jax import lax
from jax.experimental import pallas as pl
from jax.experimental.pallas import tpu as pltpu
from jax.sharding import PartitionSpec as P

residual_scale = 1.4142135
norm_eps = 1e-05
MESH = pl.DeviceIdType.MESH
LANES = 128


def kernel(n, num_tp, tokens, routes, weights, gain, bias, wg_hbm, wu_hbm, wd_hbm, out,
           xs, wg, wu, wd, own, part_out, part_in, y_out, y_in, ret_out, ret_in,
           table_out, table_in, stat_out, stat_in,
           w_sem, gs, gr, ys, yr, fs, fr, ps, pr, vs, vr, rs, rr, ts, tr, ss, sr):
    me = lax.axis_index("ep")
    core = lax.axis_index("tp")
    other = lax.rem(core + 1, num_tp)
    rows, width = tokens.shape
    half = width // num_tp
    share = rows // num_tp
    pairs = n // 2
    z, y = me // 2, lax.rem(me, 2)
    partner = 2 * z + 1 - y
    my_rows = pl.ds(pl.multiple_of(core * share, share), share)
    my_cols = pl.ds(pl.multiple_of(core * half, half), half)
    other_cols = pl.ds(pl.multiple_of(other * half, half), half)

    loads = [pltpu.make_async_copy(a.at[0], b, w_sem.at[i])
             for i, (a, b) in enumerate(((wg_hbm, wg), (wu_hbm, wu), (wd_hbm, wd)))]
    for load in loads:
        load.start()

    barrier = pltpu.get_barrier_semaphore()
    for k in range(1, n):
        pl.semaphore_signal(barrier, inc=1, device_id={"ep": lax.rem(me + k, n)}, device_id_type=MESH)
    pl.semaphore_signal(barrier, inc=1, device_id={"tp": other}, device_id_type=MESH)
    xs[me] = tokens[...]
    expert = lax.broadcasted_iota(jnp.int32, (n, rows), 0)
    table = jnp.zeros((n, rows), jnp.float32)
    for k in range(routes.shape[0]):
        table = table + jnp.where(routes[k:k + 1, :] == expert, weights[k:k + 1, :], 0.0)
    table_out[...] = table
    table_in[me] = table
    pl.semaphore_wait(barrier, n)

    def mate(g):
        total = 0
        bit = 1
        while bit < pairs:
            total = total + bit * lax.rem(z // bit + g // bit, 2)
            bit *= 2
        return total

    def own_copy():
        return pltpu.make_async_remote_copy(
            src_ref=tokens.at[my_rows, :], dst_ref=xs.at[me, my_rows, :],
            send_sem=ys.at[z], recv_sem=yr.at[z],
            device_id={"ep": partner}, device_id_type=MESH)

    def gather_copy(there, source):
        return pltpu.make_async_remote_copy(
            src_ref=tokens.at[my_rows, :], dst_ref=xs.at[2 * source + y, my_rows, :],
            send_sem=gs.at[there], recv_sem=gr.at[source],
            device_id={"ep": 2 * there + y}, device_id_type=MESH)

    def across_copy(zz, side):
        return pltpu.make_async_remote_copy(
            src_ref=xs.at[2 * zz + side, my_rows, :], dst_ref=xs.at[2 * zz + side, my_rows, :],
            send_sem=ys.at[zz], recv_sem=yr.at[zz],
            device_id={"ep": partner}, device_id_type=MESH)

    def forward_copy(source, who):
        part = pl.ds(pl.multiple_of(who * share, share), share)
        return pltpu.make_async_remote_copy(
            src_ref=xs.at[source, part, :], dst_ref=xs.at[source, part, :],
            send_sem=fs.at[source], recv_sem=fr.at[source],
            device_id={"tp": other}, device_id_type=MESH)

    def partial_copy(zz):
        block = pl.ds(2 * zz, 2)
        return pltpu.make_async_remote_copy(
            src_ref=part_out.at[block], dst_ref=part_in.at[block],
            send_sem=ps.at[zz], recv_sem=pr.at[zz],
            device_id={"tp": other}, device_id_type=MESH)

    def back_copy(zz):
        return pltpu.make_async_remote_copy(
            src_ref=y_out.at[zz], dst_ref=y_in.at[zz],
            send_sem=vs.at[zz], recv_sem=vr.at[zz],
            device_id={"ep": partner}, device_id_type=MESH)

    def return_copy(there, source):
        return pltpu.make_async_remote_copy(
            src_ref=ret_out.at[there], dst_ref=ret_in.at[source],
            send_sem=rs.at[there], recv_sem=rr.at[source],
            device_id={"ep": 2 * there + y}, device_id_type=MESH)

    def table_copy(there, source):
        return pltpu.make_async_remote_copy(
            src_ref=table_out, dst_ref=table_in.at[source],
            send_sem=ts.at[there], recv_sem=tr.at[source],
            device_id={"ep": there}, device_id_type=MESH)

    own_copy().start()
    for g in range(1, pairs):
        gather_copy(mate(g), z).start()
    for k in range(1, n):
        table_copy(lax.rem(me + k, n), me).start()

    diagonal = (lax.broadcasted_iota(jnp.int32, (rows, rows), 0)
                == lax.broadcasted_iota(jnp.int32, (rows, rows), 1))

    def weight_of(source):
        row = table_in[source, pl.ds(me, 1), :]
        return jnp.sum(jnp.where(diagonal, row, 0.0), axis=1, keepdims=True)

    def step(i, carry):
        @pl.when((i > 0) & (i < pairs))
        def _():
            zz = mate(i)
            gather_copy(zz, zz).wait_recv()
            across_copy(zz, y).start()
            forward_copy(2 * zz + y, core).start()

        @pl.when((i > 0) & (i <= pairs))
        def _():
            zz = mate(i - 1)
            across_copy(zz, 1 - y).wait_recv()
            forward_copy(2 * zz + 1 - y, core).start()

        @pl.when(i == 2)
        def _():
            for load in loads:
                load.wait()
            forward_copy(partner, other).wait_recv()

        @pl.when((i > 2) & (i <= pairs + 1))
        def _():
            zz = mate(i - 2)
            forward_copy(2 * zz, other).wait_recv()
            forward_copy(2 * zz + 1, other).wait_recv()

        @pl.when((i > 1) & (i <= pairs + 1))
        def _():
            zz = mate(i - 2)
            block = pl.ds(2 * zz, 2)
            x = xs[block].reshape(2 * rows, width)
            gate = jnp.dot(x, wg[...], preferred_element_type=jnp.float32)
            upper = jnp.dot(x, wu[...], preferred_element_type=jnp.float32)
            hidden = (gate / (1.0 + jnp.exp(-gate)) * upper).astype(jnp.bfloat16)
            theirs = jnp.dot(hidden, wd[:, other_cols], preferred_element_type=jnp.float32)
            part_out[block] = theirs.astype(jnp.bfloat16).reshape(2, rows, half)
            partial_copy(zz).start()
            mine = jnp.dot(hidden, wd[:, my_cols], preferred_element_type=jnp.float32)
            own[block] = mine.reshape(2, rows, half)

        @pl.when(i == 3)
        def _():
            table_copy(partner, partner).wait_recv()

        @pl.when((i > 3) & (i <= pairs + 2))
        def _():
            zz = mate(i - 3)
            table_copy(partner, 2 * zz).wait_recv()
            table_copy(partner, 2 * zz + 1).wait_recv()

        @pl.when((i > 2) & (i <= pairs + 2))
        def _():
            zz = mate(i - 3)
            partial_copy(zz).wait_recv()
            away = 2 * zz + 1 - y
            total = own[away] + part_in[away].astype(jnp.float32)
            y_out[zz] = (total * weight_of(away)).astype(jnp.bfloat16)
            back_copy(zz).start()
            here = 2 * zz + y
            total = own[here] + part_in[here].astype(jnp.float32)
            own[here] = total * weight_of(here)

        @pl.when(i > 3)
        def _():
            zz = mate(i - 4)
            here = 2 * zz + y
            back_copy(zz).wait_recv()
            total = own[here] + y_in[zz].astype(jnp.float32)
            own[here] = total
            ret_out[zz] = total.astype(jnp.bfloat16)

        @pl.when(i > 4)
        def _():
            return_copy(mate(i - 4), z).start()

        return carry

    lax.fori_loop(0, pairs + 4, step, 0)

    def collect(g, total):
        zz = mate(g)
        return_copy(zz, zz).wait_recv()
        return total + ret_in[zz].astype(jnp.float32)

    mixture = own[me]
    for g in range(1, pairs):
        mixture = collect(g, mixture)
    mixture = mixture.astype(jnp.bfloat16).astype(jnp.float32)
    summed = residual_scale * tokens[:, my_cols].astype(jnp.float32) + mixture
    row_sum = jnp.sum(summed, axis=1, keepdims=True)
    row_squares = jnp.sum(summed * summed, axis=1, keepdims=True)
    lane = lax.broadcasted_iota(jnp.int32, (rows, LANES), 1)
    stat_out[...] = jnp.where(lane == 0, row_sum, row_squares)
    stats = pltpu.make_async_remote_copy(
        src_ref=stat_out, dst_ref=stat_in, send_sem=ss, recv_sem=sr,
        device_id={"tp": other}, device_id_type=MESH)
    stats.start()

    own_copy().wait_send()
    forward_copy(partner, core).wait_send()
    partial_copy(z).wait_send()
    back_copy(z).wait_send()
    table_copy(partner, me).wait_send()

    def drain(g, carry):
        zz = mate(g)
        gather_copy(zz, z).wait_send()
        across_copy(zz, y).wait_send()
        partial_copy(zz).wait_send()
        back_copy(zz).wait_send()
        return_copy(zz, z).wait_send()
        for j in range(2):
            forward_copy(2 * zz + j, core).wait_send()
            table_copy(2 * zz + j, me).wait_send()
        return carry

    lax.fori_loop(1, pairs, drain, 0)
    stats.wait()
    row_sum = row_sum + stat_in[:, 0:1]
    row_squares = row_squares + stat_in[:, 1:2]
    mean = row_sum / width
    variance = row_squares / width - mean * mean
    normed = (summed - mean) * lax.rsqrt(variance + norm_eps) * gain[...] + bias[...]
    out[...] = normed.astype(jnp.bfloat16)


def shards(n, num_tp, tokens, routes, gate_weights, w_gate, w_up, w_down, norm_gain, norm_bias):
    rows, width = tokens.shape
    hidden = w_gate.shape[2]
    half = width // num_tp
    pairs = n // 2
    vmem = pl.BlockSpec(memory_space=pltpu.VMEM)
    hbm = pl.BlockSpec(memory_space=pl.ANY)
    dma = pltpu.SemaphoreType.DMA
    return pl.pallas_call(
        functools.partial(kernel, n, num_tp),
        out_shape=jax.ShapeDtypeStruct((rows, half), jnp.bfloat16),
        in_specs=[vmem] * 5 + [hbm] * 3,
        out_specs=vmem,
        scratch_shapes=[
            pltpu.VMEM((n, rows, width), jnp.bfloat16),
            pltpu.VMEM((width, hidden), jnp.bfloat16),
            pltpu.VMEM((width, hidden), jnp.bfloat16),
            pltpu.VMEM((hidden, width), jnp.bfloat16),
            pltpu.VMEM((n, rows, half), jnp.float32),
            pltpu.VMEM((n, rows, half), jnp.bfloat16),
            pltpu.VMEM((n, rows, half), jnp.bfloat16),
            pltpu.VMEM((pairs, rows, half), jnp.bfloat16),
            pltpu.VMEM((pairs, rows, half), jnp.bfloat16),
            pltpu.VMEM((pairs, rows, half), jnp.bfloat16),
            pltpu.VMEM((pairs, rows, half), jnp.bfloat16),
            pltpu.VMEM((n, rows), jnp.float32),
            pltpu.VMEM((n, n, rows), jnp.float32),
            pltpu.VMEM((rows, LANES), jnp.float32),
            pltpu.VMEM((rows, LANES), jnp.float32),
            dma((3,)), dma((pairs,)), dma((pairs,)), dma((pairs,)), dma((pairs,)), dma((n,)), dma((n,)),
            dma((pairs,)), dma((pairs,)), dma((pairs,)), dma((pairs,)), dma((pairs,)), dma((pairs,)),
            dma((n,)), dma((n,)), dma, dma,
        ],
        compiler_params=pltpu.CompilerParams(collective_id=0, has_side_effects=True),
    )(tokens, routes.T, gate_weights.T, norm_gain.reshape(1, half), norm_bias.reshape(1, half),
      w_gate, w_up, w_down)


def solution(mesh):
    in_specs = (
        P(("grp", "ep"), None),
        P(("grp", "ep"), None),
        P(("grp", "ep"), None),
        P("ep", None, "tp"),
        P("ep", None, "tp"),
        P("ep", "tp", None),
        P("tp"),
        P("tp"),
    )
    out_specs = P(("grp", "ep"), "tp")
    body = functools.partial(shards, mesh.shape["ep"], mesh.shape["tp"])
    return jax.shard_map(body, mesh=mesh, in_specs=in_specs, out_specs=out_specs, check_vma=False)
```

```python
import functools
import jax
import jax.numpy as jnp
from jax import lax
from jax.experimental import pallas as pl
from jax.experimental.pallas import tpu as pltpu
from jax.sharding import PartitionSpec as P

residual_scale = 1.4142135
norm_eps = 1e-05
MESH = pl.DeviceIdType.MESH
LANES = 128
CHUNKS = 2


def kernel(n, num_tp, tokens, routes, weights, gain, bias, wg_hbm, wu_hbm, wd_hbm, out,
           xs, wg, wu, wd, own, part_out, part_in, y_out, y_in, ret_out, ret_in,
           table_out, table_in, stat_out, stat_in,
           w_sem, gs, gr, ys, yr, fs, fr, ps, pr, vs, vr, rs, rr, ts, tr, ss, sr):
    me = lax.axis_index("ep")
    core = lax.axis_index("tp")
    other = lax.rem(core + 1, num_tp)
    rows, width = tokens.shape
    half = width // num_tp
    share = rows // num_tp
    pairs = n // 2
    z, y = me // 2, lax.rem(me, 2)
    partner = 2 * z + 1 - y
    my_cols = pl.ds(pl.multiple_of(core * half, half), half)
    other_cols = pl.ds(pl.multiple_of(other * half, half), half)

    loads = [pltpu.make_async_copy(a.at[0], b, w_sem.at[i])
             for i, (a, b) in enumerate(((wg_hbm, wg), (wu_hbm, wu), (wd_hbm, wd)))]
    for load in loads:
        load.start()

    barrier = pltpu.get_barrier_semaphore()
    for k in range(1, n):
        pl.semaphore_signal(barrier, inc=1, device_id={"ep": lax.rem(me + k, n)}, device_id_type=MESH)
    pl.semaphore_signal(barrier, inc=1, device_id={"tp": other}, device_id_type=MESH)
    xs[me] = tokens[...]
    expert = lax.broadcasted_iota(jnp.int32, (n, rows), 0)
    table = jnp.zeros((n, rows), jnp.float32)
    for k in range(routes.shape[0]):
        table = table + jnp.where(routes[k:k + 1, :] == expert, weights[k:k + 1, :], 0.0)
    table_out[...] = table
    table_in[me] = table
    pl.semaphore_wait(barrier, n)

    def mate(g):
        total = 0
        bit = 1
        while bit < pairs:
            total = total + bit * lax.rem(z // bit + g // bit, 2)
            bit *= 2
        return total

    def my_chunk(c):
        chunk = share // CHUNKS
        return pl.ds(pl.multiple_of(core * share + c * chunk, chunk), chunk)

    def chunk_of(c):
        chunk = rows // CHUNKS
        return pl.ds(c * chunk, chunk)

    def own_copy(c):
        return pltpu.make_async_remote_copy(
            src_ref=tokens.at[my_chunk(c), :], dst_ref=xs.at[me, my_chunk(c), :],
            send_sem=ys.at[z, c], recv_sem=yr.at[z, c],
            device_id={"ep": partner}, device_id_type=MESH)

    def gather_copy(there, source, c):
        return pltpu.make_async_remote_copy(
            src_ref=tokens.at[my_chunk(c), :], dst_ref=xs.at[2 * source + y, my_chunk(c), :],
            send_sem=gs.at[there, c], recv_sem=gr.at[source, c],
            device_id={"ep": 2 * there + y}, device_id_type=MESH)

    def across_copy(zz, side, c):
        return pltpu.make_async_remote_copy(
            src_ref=xs.at[2 * zz + side, my_chunk(c), :], dst_ref=xs.at[2 * zz + side, my_chunk(c), :],
            send_sem=ys.at[zz, c], recv_sem=yr.at[zz, c],
            device_id={"ep": partner}, device_id_type=MESH)

    def forward_copy(source, who):
        part = pl.ds(pl.multiple_of(who * share, share), share)
        return pltpu.make_async_remote_copy(
            src_ref=xs.at[source, part, :], dst_ref=xs.at[source, part, :],
            send_sem=fs.at[source], recv_sem=fr.at[source],
            device_id={"tp": other}, device_id_type=MESH)

    def partial_copy(zz):
        block = pl.ds(2 * zz, 2)
        return pltpu.make_async_remote_copy(
            src_ref=part_out.at[block], dst_ref=part_in.at[block],
            send_sem=ps.at[zz], recv_sem=pr.at[zz],
            device_id={"tp": other}, device_id_type=MESH)

    def back_copy(zz, c):
        return pltpu.make_async_remote_copy(
            src_ref=y_out.at[zz, chunk_of(c), :], dst_ref=y_in.at[zz, chunk_of(c), :],
            send_sem=vs.at[zz, c], recv_sem=vr.at[zz, c],
            device_id={"ep": partner}, device_id_type=MESH)

    def return_copy(there, source, c):
        return pltpu.make_async_remote_copy(
            src_ref=ret_out.at[there, chunk_of(c), :], dst_ref=ret_in.at[source, chunk_of(c), :],
            send_sem=rs.at[there, c], recv_sem=rr.at[source, c],
            device_id={"ep": 2 * there + y}, device_id_type=MESH)

    def table_copy(there, source):
        return pltpu.make_async_remote_copy(
            src_ref=table_out, dst_ref=table_in.at[source],
            send_sem=ts.at[there], recv_sem=tr.at[source],
            device_id={"ep": there}, device_id_type=MESH)

    for c in range(CHUNKS):
        own_copy(c).start()
    for g in range(1, pairs):
        for c in range(CHUNKS):
            gather_copy(mate(g), z, c).start()
    for k in range(1, n):
        table_copy(lax.rem(me + k, n), me).start()

    diagonal = (lax.broadcasted_iota(jnp.int32, (rows, rows), 0)
                == lax.broadcasted_iota(jnp.int32, (rows, rows), 1))

    def weight_of(source):
        row = table_in[source, pl.ds(me, 1), :]
        return jnp.sum(jnp.where(diagonal, row, 0.0), axis=1, keepdims=True)

    def step(i, carry):
        @pl.when((i > 0) & (i < pairs))
        def _():
            zz = mate(i)
            for c in range(CHUNKS):
                gather_copy(zz, zz, c).wait_recv()
                across_copy(zz, y, c).start()
            forward_copy(2 * zz + y, core).start()

        @pl.when((i > 0) & (i <= pairs))
        def _():
            zz = mate(i - 1)
            for c in range(CHUNKS):
                across_copy(zz, 1 - y, c).wait_recv()
            forward_copy(2 * zz + 1 - y, core).start()

        @pl.when(i == 1)
        def _():
            for load in loads:
                load.wait()
            forward_copy(partner, other).wait_recv()

        @pl.when((i > 1) & (i <= pairs))
        def _():
            zz = mate(i - 1)
            forward_copy(2 * zz, other).wait_recv()
            forward_copy(2 * zz + 1, other).wait_recv()

        @pl.when((i > 0) & (i <= pairs))
        def _():
            zz = mate(i - 1)
            block = pl.ds(2 * zz, 2)
            x = xs[block].reshape(2 * rows, width)
            gate = jnp.dot(x, wg[...], preferred_element_type=jnp.float32)
            upper = jnp.dot(x, wu[...], preferred_element_type=jnp.float32)
            hidden = (gate / (1.0 + jnp.exp(-gate)) * upper).astype(jnp.bfloat16)
            theirs = jnp.dot(hidden, wd[:, other_cols], preferred_element_type=jnp.float32)
            part_out[block] = theirs.astype(jnp.bfloat16).reshape(2, rows, half)
            partial_copy(zz).start()
            mine = jnp.dot(hidden, wd[:, my_cols], preferred_element_type=jnp.float32)
            own[block] = mine.reshape(2, rows, half)

        @pl.when(i == 1)
        def _():
            table_copy(partner, partner).wait_recv()

        @pl.when((i > 1) & (i <= pairs))
        def _():
            zz = mate(i - 1)
            table_copy(partner, 2 * zz).wait_recv()
            table_copy(partner, 2 * zz + 1).wait_recv()

        @pl.when((i > 0) & (i <= pairs))
        def _():
            zz = mate(i - 1)
            partial_copy(zz).wait_recv()
            away = 2 * zz + 1 - y
            total = own[away] + part_in[away].astype(jnp.float32)
            y_out[zz] = (total * weight_of(away)).astype(jnp.bfloat16)
            for c in range(CHUNKS):
                back_copy(zz, c).start()
            here = 2 * zz + y
            total = own[here] + part_in[here].astype(jnp.float32)
            own[here] = total * weight_of(here)

        @pl.when(i == 2)
        def _():
            for c in range(CHUNKS):
                back_copy(z, c).wait_recv()
            own[me] = own[me] + y_in[z].astype(jnp.float32)

        @pl.when(i > 2)
        def _():
            zz = mate(i - 2)
            here = 2 * zz + y
            for c in range(CHUNKS):
                back_copy(zz, c).wait_recv()
                total = own[here, chunk_of(c), :] + y_in[zz, chunk_of(c), :].astype(jnp.float32)
                ret_out[zz, chunk_of(c), :] = total.astype(jnp.bfloat16)
                return_copy(zz, z, c).start()

        return carry

    lax.fori_loop(1, pairs + 2, step, 0)

    def collect(g, total):
        zz = mate(g)
        for c in range(CHUNKS):
            return_copy(zz, zz, c).wait_recv()
        return total + ret_in[zz].astype(jnp.float32)

    mixture = own[me]
    for g in range(1, pairs):
        mixture = collect(g, mixture)
    mixture = mixture.astype(jnp.bfloat16).astype(jnp.float32)
    summed = residual_scale * tokens[:, my_cols].astype(jnp.float32) + mixture
    row_sum = jnp.sum(summed, axis=1, keepdims=True)
    row_squares = jnp.sum(summed * summed, axis=1, keepdims=True)
    lane = lax.broadcasted_iota(jnp.int32, (rows, LANES), 1)
    stat_out[...] = jnp.where(lane == 0, row_sum, row_squares)
    stats = pltpu.make_async_remote_copy(
        src_ref=stat_out, dst_ref=stat_in, send_sem=ss, recv_sem=sr,
        device_id={"tp": other}, device_id_type=MESH)
    stats.start()

    for c in range(CHUNKS):
        own_copy(c).wait_send()
        back_copy(z, c).wait_send()
    forward_copy(partner, core).wait_send()
    partial_copy(z).wait_send()
    table_copy(partner, me).wait_send()

    def drain(g, carry):
        zz = mate(g)
        partial_copy(zz).wait_send()
        for c in range(CHUNKS):
            gather_copy(zz, z, c).wait_send()
            across_copy(zz, y, c).wait_send()
            back_copy(zz, c).wait_send()
            return_copy(zz, z, c).wait_send()
        for j in range(2):
            forward_copy(2 * zz + j, core).wait_send()
            table_copy(2 * zz + j, me).wait_send()
        return carry

    lax.fori_loop(1, pairs, drain, 0)
    stats.wait()
    row_sum = row_sum + stat_in[:, 0:1]
    row_squares = row_squares + stat_in[:, 1:2]
    mean = row_sum / width
    variance = row_squares / width - mean * mean
    normed = (summed - mean) * lax.rsqrt(variance + norm_eps) * gain[...] + bias[...]
    out[...] = normed.astype(jnp.bfloat16)


def shards(n, num_tp, tokens, routes, gate_weights, w_gate, w_up, w_down, norm_gain, norm_bias):
    rows, width = tokens.shape
    hidden = w_gate.shape[2]
    half = width // num_tp
    pairs = n // 2
    vmem = pl.BlockSpec(memory_space=pltpu.VMEM)
    hbm = pl.BlockSpec(memory_space=pl.ANY)
    dma = pltpu.SemaphoreType.DMA
    hop = dma((pairs, CHUNKS))
    return pl.pallas_call(
        functools.partial(kernel, n, num_tp),
        out_shape=jax.ShapeDtypeStruct((rows, half), jnp.bfloat16),
        in_specs=[vmem] * 5 + [hbm] * 3,
        out_specs=vmem,
        scratch_shapes=[
            pltpu.VMEM((n, rows, width), jnp.bfloat16),
            pltpu.VMEM((width, hidden), jnp.bfloat16),
            pltpu.VMEM((width, hidden), jnp.bfloat16),
            pltpu.VMEM((hidden, width), jnp.bfloat16),
            pltpu.VMEM((n, rows, half), jnp.float32),
            pltpu.VMEM((n, rows, half), jnp.bfloat16),
            pltpu.VMEM((n, rows, half), jnp.bfloat16),
            pltpu.VMEM((pairs, rows, half), jnp.bfloat16),
            pltpu.VMEM((pairs, rows, half), jnp.bfloat16),
            pltpu.VMEM((pairs, rows, half), jnp.bfloat16),
            pltpu.VMEM((pairs, rows, half), jnp.bfloat16),
            pltpu.VMEM((n, rows), jnp.float32),
            pltpu.VMEM((n, n, rows), jnp.float32),
            pltpu.VMEM((rows, LANES), jnp.float32),
            pltpu.VMEM((rows, LANES), jnp.float32),
            dma((3,)), hop, hop, hop, hop, dma((n,)), dma((n,)),
            dma((pairs,)), dma((pairs,)), hop, hop, hop, hop,
            dma((n,)), dma((n,)), dma, dma,
        ],
        compiler_params=pltpu.CompilerParams(collective_id=0, has_side_effects=True),
    )(tokens, routes.T, gate_weights.T, norm_gain.reshape(1, half), norm_bias.reshape(1, half),
      w_gate, w_up, w_down)


def solution(mesh):
    in_specs = (
        P(("grp", "ep"), None),
        P(("grp", "ep"), None),
        P(("grp", "ep"), None),
        P("ep", None, "tp"),
        P("ep", None, "tp"),
        P("ep", "tp", None),
        P("tp"),
        P("tp"),
    )
    out_specs = P(("grp", "ep"), "tp")
    body = functools.partial(shards, mesh.shape["ep"], mesh.shape["tp"])
    return jax.shard_map(body, mesh=mesh, in_specs=in_specs, out_specs=out_specs, check_vma=False)
```
